32 devices in a mesh: sp: 8 (over z, x), tp: 4 (over y, core).
Axes of the slice: x: 2, y: 2, z: 4, core: 2. Of those that a mesh axis runs over, the one named last changes fastest.
Arguments:
- queries: bfloat16 [8192, 2048], P('sp', 'tp'), may hold values from -16 to 16
- key_rows: bfloat16 [8192, 512], P('sp', 'tp'), may hold values from -16 to 16
- value_rows: bfloat16 [8192, 512], P('sp', 'tp'), may hold values from -6 to 6
- doc_ids: int32 [8192], P('sp'), may hold values from 0 to 3, never falling along the last dimension, each value on 1 to 4096 neighbouring positions
- sink_logit: float32 [32], P('tp'), may hold values from 3 to 7
- residual: bfloat16 [8192, 2048], P(('sp', 'tp')), may hold values from -6 to 6
- out_weight: bfloat16 [2048, 2048], P('tp'), may hold values from -3.5 to 3.5
- norm_gain: float32 [2048], replicated, may hold values from 0.1 to 1.9
- gate_weight: bfloat16 [8, 2048, 512], P('sp'), may hold values from -0.125 to 0.125
- up_weight: bfloat16 [8, 2048, 512], P('sp'), may hold values from -0.125 to 0.125
- down_weight: bfloat16 [8, 512, 2048], P('sp'), may hold values from -0.25 to 0.25
- routes: int32 [8192, 2], P(('sp', 'tp')), may hold values from 0 to 7, as said below
- route_weights: float32 [8192, 2], P(('sp', 'tp')), may hold values from 0.2 to 0.8
Outputs:
- mixed: bfloat16 [8192, 2048], P(('sp', 'tp'))
The draws below stay inside these ranges and needn't reach their ends.
Inputs may be any that keep to these rules, and one draw needn't show every extreme that they name: `doc_ids`: never falls along the positions. `routes`: each aligned block of 256 rows names every expert exactly 64 times; the experts of one row differ and lie in one group of 2 consecutive numbers.
All inputs are finite; a program needn't handle non-finite values.
Results may differ from the reference program's by a relative error of at most 0.012.
Values may be sent and summed in bfloat16 or wider, within the bound.
A program may use at most 128 MiB of HBM per device.

```python
import math
import jax
import jax.numpy as jnp
import numpy as np
from jax import lax

D = 2048
HEADS = 32
KV_HEADS = 8
HD = 64
FF = 512
WINDOW = 128
GROUPS = 4
TOPK = 2
TOKENS = 8192
EXPERTS = 8
GROUP_SIZE = 2
ROWS_HOME = 256
CAP = 64
DOCS = 4
DOC_MOST = 4096
N_TP = 4


def draw_queries(key, part):
    noise = jax.random.truncated_normal(jax.random.fold_in(key, 11), -4.0, 4.0, (TOKENS, HEADS * HD), jnp.float32)
    return noise.astype(jnp.bfloat16)


def draw_key_rows(key, part):
    noise = jax.random.truncated_normal(jax.random.fold_in(key, 12), -4.0, 4.0, (TOKENS, KV_HEADS * HD), jnp.float32)
    return noise.astype(jnp.bfloat16)


def draw_routes(key, part):
    block_total = TOKENS // ROWS_HOME
    half_slots = GROUP_SIZE * CAP // 2

    def one_block(block_key):
        order_key, shuffle_key = jax.random.split(block_key)
        group_keys = jax.random.split(order_key, GROUPS)
        ordering = jax.vmap(lambda group_key: jax.random.permutation(group_key, GROUP_SIZE))(group_keys)
        ordering = ordering.astype(jnp.int32) + (jnp.arange(GROUPS, dtype=jnp.int32) * GROUP_SIZE)[:, None]
        slot_ids = jnp.arange(half_slots, dtype=jnp.int32)
        leading = ordering[:, slot_ids // CAP]
        trailing = ordering[:, (slot_ids + half_slots) // CAP]
        paired = jnp.stack([leading.reshape(-1), trailing.reshape(-1)], axis=1)
        shuffle = jax.random.permutation(shuffle_key, ROWS_HOME)
        return paired[shuffle].astype(jnp.int32)
    blocks = jax.vmap(one_block)(jax.random.split(jax.random.fold_in(key, 77), block_total))
    return blocks.reshape(TOKENS, TOPK)


def levels(key, shape, cuts, low, high):
    gain, own = 1.0, jax.random.fold_in(key, 6)
    for dim, blocks in cuts:
        draws = jnp.exp(jax.random.uniform(jax.random.fold_in(own, dim), (blocks,), jnp.float32, low / len(cuts), high / len(cuts)))
        gain = gain * jnp.repeat(draws, shape[dim] // blocks).reshape([-1 if axis == dim else 1 for axis in range(len(shape))])
    return gain


def split_up(number_of, total, limit, lean):
    portions = [(1 << 20) // math.isqrt(standing ** lean) + 1 for standing in range(2, number_of + 1)]
    rest, counts = total - limit - (number_of - 1), [1] * (number_of - 1)
    while rest > 0:
        candidates = [i for i in range(number_of - 1) if counts[i] < limit]
        whole, remaining = sum([portions[i] for i in candidates]), rest
        for i in candidates:
            extra = min(limit - counts[i], max(1, remaining * portions[i] // whole), rest)
            counts[i] = counts[i] + extra
            rest = rest - extra
    return np.array([limit] + counts)


def uneven(own_key, number_of, total, bound, skew):
    if number_of == 2:
        one = jax.random.randint(own_key, (), max(1, total - bound), min(bound, total - 1) + 1)
        return jnp.stack([one, total - one])
    lengths = jnp.asarray(split_up(number_of, total, bound, skew), jnp.int32)
    pairs = (number_of - 1) // 2
    giver, taker = lengths[1:1 + 2 * pairs:2], lengths[2:2 + 2 * pairs:2]
    margin = jnp.minimum(giver - 1, bound - taker)
    moved = jax.random.randint(jax.random.fold_in(own_key, 1), (pairs,), 0, 1 << 20) % (margin + 1)
    lengths = lengths.at[1:1 + 2 * pairs:2].set(giver - moved).at[2:2 + 2 * pairs:2].set(taker + moved)
    return lengths[jax.random.permutation(jax.random.fold_in(own_key, 2), number_of)]


def normal_values(key, extent, width, most, pieces=(), kind=jnp.bfloat16):
    factor_of = levels(key, extent, pieces, -0.22, 0.18) if pieces else 1.0
    values = jax.random.normal(key, extent, jnp.float32) * width * factor_of
    return jnp.minimum(jnp.maximum(values, -most), most).astype(kind)


def setup_inputs(seed: int = 0) -> dict:
    keys = jax.random.split(jax.random.key(seed), 14)
    queries = draw_queries(jax.random.fold_in(keys[13], 71), 0)
    key_rows = draw_key_rows(jax.random.fold_in(keys[13], 71), 0)
    value_rows = normal_values(keys[2], (TOKENS, KV_HEADS * HD), 1.0, 6.0, ((0, 8), (1, 4)))
    doc_ids = jnp.searchsorted(jnp.cumsum(uneven(keys[3], DOCS, TOKENS, DOC_MOST, 1)), jnp.arange(TOKENS), side="right").astype(jnp.int32)
    sink_logit = jnp.clip(3.0 + 4.0 * jax.random.uniform(keys[4], (HEADS,), jnp.float32) ** levels(keys[4], (HEADS,), ((0, 4),), -0.2, 0.2), 3.0, 7.0)
    residual = normal_values(keys[5], (TOKENS, D), 1.0, 6.0, ((0, 32),))
    out_weight = normal_values(keys[6], (HEADS * HD, D), ((HEADS * HD) ** -0.5 * 10), 3.5, ((0, 4),))
    norm_gain = jnp.clip(1.0 + 0.18 * jax.random.normal(keys[7], (D,), jnp.float32), 0.1, 1.9)
    gate_weight = normal_values(keys[8], (EXPERTS, D, FF), D ** -0.5, 0.125, ((0, 8),))
    up_weight = normal_values(keys[9], (EXPERTS, D, FF), D ** -0.5, 0.125, ((0, 8),))
    down_weight = normal_values(keys[10], (EXPERTS, FF, D), FF ** -0.5, 0.25, ((0, 8),))
    routes = draw_routes(jax.random.fold_in(keys[13], 71), 0)
    route_weights = jnp.clip(0.2 + 0.6 * jax.random.uniform(keys[12], (TOKENS, TOPK), jnp.float32) ** levels(keys[12], (TOKENS, TOPK), ((0, 32),), -0.2, 0.2), 0.2, 0.8)
    return dict(queries=queries, key_rows=key_rows, value_rows=value_rows, doc_ids=doc_ids, sink_logit=sink_logit, residual=residual, out_weight=out_weight, norm_gain=norm_gain, gate_weight=gate_weight, up_weight=up_weight, down_weight=down_weight, routes=routes, route_weights=route_weights)


neg_fill = -1e+30
eps_norm = 1e-06

def reference(queries, key_rows, value_rows, doc_ids, sink_logit, residual, out_weight, norm_gain, gate_weight, up_weight, down_weight, routes, route_weights):
    head_ratio = HEADS // KV_HEADS
    block_rows = 512
    block_total = TOKENS // block_rows
    key_pad = jnp.pad(key_rows, ((WINDOW, WINDOW), (0, 0)))
    value_pad = jnp.pad(value_rows, ((WINDOW, WINDOW), (0, 0)))
    doc_pad = jnp.pad(doc_ids, (WINDOW, WINDOW), constant_values=-1)
    sink_col = sink_logit.astype(jnp.float32).reshape(KV_HEADS, head_ratio)[:, :, None, None]

    def one_block(block_index):
        row_start = (block_index * block_rows).astype(jnp.int32)
        key_count = block_rows + 2 * WINDOW
        query_part = lax.dynamic_slice_in_dim(queries, row_start, block_rows, 0).astype(jnp.float32)
        query_part = query_part.reshape(block_rows, KV_HEADS, head_ratio, HD)
        key_part = lax.dynamic_slice_in_dim(key_pad, row_start, key_count, 0).astype(jnp.float32).reshape(key_count, KV_HEADS, HD)
        value_part = lax.dynamic_slice_in_dim(value_pad, row_start, key_count, 0).astype(jnp.float32).reshape(key_count, KV_HEADS, HD)
        query_docs = lax.dynamic_slice_in_dim(doc_ids, row_start, block_rows, 0)
        key_docs = lax.dynamic_slice_in_dim(doc_pad, row_start, key_count, 0)
        query_pos = row_start + jnp.arange(block_rows, dtype=jnp.int32)
        key_pos = row_start - WINDOW + jnp.arange(key_count, dtype=jnp.int32)
        allowed = (jnp.abs(query_pos[:, None] - key_pos[None, :]) <= WINDOW) & (query_docs[:, None] == key_docs[None, :])
        scores = jnp.einsum('qgrd,kgd->grqk', query_part, key_part) * HD ** (-0.5)
        masked = jnp.where(allowed[None, None], scores, neg_fill)
        row_top = jnp.maximum(lax.optimization_barrier(jnp.max(masked, axis=3, keepdims=True)), sink_col)
        exponent = jnp.where(allowed[None, None], jnp.exp(masked - row_top), 0.0)
        denominator = lax.optimization_barrier(jnp.sum(exponent, axis=3, keepdims=True)) + jnp.exp(sink_col - row_top)
        attn_weight = (exponent / denominator).astype(jnp.bfloat16)
        attended = jnp.einsum('grqk,kgd->qgrd', attn_weight.astype(jnp.float32), value_part)
        return attended.astype(jnp.bfloat16).reshape(block_rows, HEADS * HD)
    attended = lax.map(one_block, jnp.arange(block_total, dtype=jnp.int32)).reshape(TOKENS, HEADS * HD)
    group_cols = HEADS * HD // N_TP
    summed = jnp.zeros((TOKENS, D), jnp.float32)
    for group_index in range(N_TP):
        cols = attended[:, group_index * group_cols:(group_index + 1) * group_cols]
        rows_w = out_weight[group_index * group_cols:(group_index + 1) * group_cols]
        partial_value = jnp.dot(cols, rows_w, preferred_element_type=jnp.float32).astype(jnp.bfloat16)
        partial_value = lax.optimization_barrier(partial_value)
        summed = summed + partial_value.astype(jnp.float32)
    stream = (residual.astype(jnp.float32) + summed).astype(jnp.bfloat16)
    stream_f = stream.astype(jnp.float32)
    scale = lax.rsqrt(lax.optimization_barrier(jnp.mean(stream_f * stream_f, axis=1, keepdims=True)) + eps_norm)
    normed = (stream_f * scale * norm_gain.astype(jnp.float32)[None, :]).astype(jnp.bfloat16)
    flat_routes = routes.reshape(-1)
    flat_weights = route_weights.reshape(-1).astype(jnp.float32)
    per_expert = TOKENS * TOPK // EXPERTS

    def expert_step(accum, inputs):
        expert_id, gate_one, up_one, down_one = inputs
        found = jnp.nonzero(flat_routes == expert_id, size=per_expert)[0].astype(jnp.int32)
        token_index = found // TOPK
        rows = normed[token_index]
        gate_act = jnp.dot(rows, gate_one, preferred_element_type=jnp.float32)
        up_act = jnp.dot(rows, up_one, preferred_element_type=jnp.float32)
        hidden = (jax.nn.silu(gate_act) * up_act).astype(jnp.bfloat16)
        expert_out = jnp.dot(hidden, down_one, preferred_element_type=jnp.float32).astype(jnp.bfloat16)
        accum = accum.at[token_index].add(flat_weights[found][:, None] * expert_out.astype(jnp.float32))
        return (accum, None)
    accum0 = jnp.zeros((TOKENS, D), jnp.float32)
    accum, _ = lax.scan(expert_step, accum0, (jnp.arange(EXPERTS, dtype=jnp.int32), gate_weight, up_weight, down_weight))
    return (stream_f + accum).astype(jnp.bfloat16)
```

```python
import functools

import jax
import jax.numpy as jnp
from jax import lax
from jax.experimental import pallas as pl
from jax.experimental.pallas import tpu as pltpu
from jax.sharding import PartitionSpec as P

HD = 64
WINDOW = 128
GROUPS = 4
CHUNKS = 4


neg_fill = -1e30
eps_norm = 1e-06


def extended(block, sides, width):
    for axis, dim in sides:
        count = lax.axis_size(axis)
        forward = [(i, i + 1) for i in range(count - 1)]
        backward = [(target, source) for source, target in forward]
        low = lax.ppermute(
            lax.slice_in_dim(block, block.shape[dim] - width, None, axis=dim), axis, forward
        )
        high = lax.ppermute(lax.slice_in_dim(block, 0, width, axis=dim), axis, backward)
        block = jnp.concatenate([low, block, high], axis=dim)
    return block


def attend(
    query_part,
    key_part,
    value_part,
    query_docs,
    key_docs,
    query_start,
    key_start,
    sink_logit,
    extent,
):
    query_count = query_part.shape[0]
    key_count = key_part.shape[0]
    groups = key_part.shape[1] // HD
    head_ratio = sink_logit.shape[0] // groups
    query_heads = query_part.reshape(query_count, groups, head_ratio, HD)
    key_heads = key_part.reshape(key_count, groups, HD)
    value_heads = value_part.reshape(key_count, groups, HD)
    scores = jnp.einsum(
        "qgrd,kgd->grqk", query_heads, key_heads, preferred_element_type=jnp.float32
    ) * HD ** (-0.5)
    query_pos = query_start + jnp.arange(query_count, dtype=jnp.int32)
    key_pos = key_start + jnp.arange(key_count, dtype=jnp.int32)
    inside = (key_pos >= 0) & (key_pos < extent)
    allowed = (
        (jnp.abs(query_pos[:, None] - key_pos[None, :]) <= WINDOW)
        & (query_docs[:, None] == key_docs[None, :])
        & inside[None, :]
    )
    masked = jnp.where(allowed[None, None], scores, neg_fill)
    sink_col = sink_logit.reshape(groups, head_ratio)[:, :, None, None]
    row_top = jnp.maximum(jnp.max(masked, axis=3, keepdims=True), sink_col)
    exponent = jnp.where(allowed[None, None], jnp.exp(masked - row_top), 0.0)
    denominator = jnp.sum(exponent, axis=3, keepdims=True) + jnp.exp(sink_col - row_top)
    attn_weight = (exponent / denominator).astype(jnp.bfloat16)
    attended = jnp.einsum(
        "grqk,kgd->qgrd", attn_weight, value_heads, preferred_element_type=jnp.float32
    )
    return attended.astype(jnp.bfloat16).reshape(query_count, -1)


def fetch_margins(key_rows, value_rows, doc_float):
    return (
        extended(key_rows, (("sp", 0),), WINDOW),
        extended(value_rows, (("sp", 0),), WINDOW),
        extended(doc_float, (("sp", 0),), WINDOW),
    )


def moe_kernel(
    groups, chunks,
    stream_ref, gain_ref, routes_ref, rw_ref, gate_hbm, up_hbm, down_hbm,
    out_ref,
    send, own, peer, pout, pin, comb, ret, wsend, wown, wpeer,
    gv, uv, dv, acc_g, acc_u,
    zs, zr, xs, xr, zws, zwr, xws, xwr, bzs, bzr, bxs, bxr, wsem,
):
    me = lax.axis_index("sp")
    gz = me // 2
    side = me % 2
    mate = gz * 2 + 1 - side
    rows, width = stream_ref.shape
    cap = rows // groups
    cw = width // chunks
    half = groups // 2
    offsets = [half] + [d for d in range(groups - 1, 0, -1) if d != half]

    def remote(src, dst, ss, rs, target):
        return pltpu.make_async_remote_copy(
            src_ref=src, dst_ref=dst, send_sem=ss, recv_sem=rs,
            device_id={"sp": target}, device_id_type=pl.DeviceIdType.MESH,
        )

    barrier = pltpu.get_barrier_semaphore()
    for d in offsets:
        pl.semaphore_signal(
            barrier, inc=1, device_id={"sp": ((gz + d) % groups) * 2 + side},
            device_id_type=pl.DeviceIdType.MESH,
        )
    pl.semaphore_signal(
        barrier, inc=1, device_id={"sp": mate}, device_id_type=pl.DeviceIdType.MESH
    )
    loads = [
        pltpu.make_async_copy(s.at[0], t, wsem.at[i])
        for i, (s, t) in enumerate(((gate_hbm, gv), (up_hbm, uv), (down_hbm, dv)))
    ]
    for load in loads:
        load.start()

    stream_f = stream_ref[...].astype(jnp.float32)
    scale = lax.rsqrt(jnp.mean(stream_f * stream_f, axis=1, keepdims=True) + eps_norm)
    normed = (stream_f * scale * gain_ref[...]).astype(jnp.bfloat16)

    first = routes_ref[:, 0:1]
    group_of = first // 2
    lanes = lax.broadcasted_iota(jnp.int32, (rows, 128), 1)
    one_hot = jnp.where(group_of == lanes, 1.0, 0.0)
    ri = lax.broadcasted_iota(jnp.int32, (rows, rows), 0)
    ci = lax.broadcasted_iota(jnp.int32, (rows, rows), 1)
    below = jnp.where(ci < ri, 1.0, 0.0).astype(jnp.bfloat16)
    ranks = jnp.dot(below, one_hot.astype(jnp.bfloat16), preferred_element_type=jnp.float32)
    slot = group_of.astype(jnp.float32) * cap + jnp.sum(ranks * one_hot, axis=1, keepdims=True)
    spread = jnp.where(slot == ci.astype(jnp.float32), 1.0, 0.0)
    spread_b = spread.astype(jnp.bfloat16)
    slot_lane = jnp.sum(jnp.where(ri == ci, slot, 0.0), axis=0, keepdims=True)
    pick = jnp.where(ri.astype(jnp.float32) == slot_lane, 1.0, 0.0).astype(jnp.bfloat16)
    for parity in range(2):
        w_col = jnp.where(first % 2 == parity, rw_ref[:, 0:1], rw_ref[:, 1:2])
        w_row = jnp.sum(spread * w_col, axis=0, keepdims=True)
        wsend[parity] = jnp.broadcast_to(w_row, (8, rows))

    pl.semaphore_wait(barrier, groups)

    pending = []
    for d in offsets:
        copy = remote(wsend, wown.at[gz], zws.at[d], zwr.at[gz], ((gz + d) % groups) * 2 + side)
        copy.start()
        pending.append(copy)
    copy = remote(wsend, wpeer.at[gz], xws.at[gz], xwr.at[gz], mate)
    copy.start()
    pending.append(copy)

    for j in range(chunks):
        piece = jnp.dot(pick, normed[:, j * cw:(j + 1) * cw], preferred_element_type=jnp.float32)
        send[j] = piece.astype(jnp.bfloat16).reshape(groups, cap, cw)
        for d in offsets:
            target = (gz + d) % groups
            copy = remote(
                send.at[j, target], own.at[j, gz], zs.at[j, d], zr.at[j, gz], target * 2 + side
            )
            copy.start()
            pending.append(copy)
        copy = remote(send.at[j, gz], peer.at[j, gz], xs.at[j, gz], xr.at[j, gz], mate)
        copy.start()
        pending.append(copy)
        own[j, pl.ds(gz, 1)] = send[j, pl.ds(gz, 1)]
    wown[pl.ds(gz, 1)] = wsend[...][None]

    for d in offsets:
        source = (gz + groups - d) % groups
        remote(wsend, wown.at[source], zws.at[d], zwr.at[source], mate).wait_recv()
        copy = remote(wown.at[source], wpeer.at[source], xws.at[source], xwr.at[source], mate)
        copy.start()
        pending.append(copy)

    loads[0].wait()
    loads[1].wait()

    def accumulate(buf, j, base):
        block = buf[j].reshape(rows, cw)
        part_g = jnp.dot(block, gv[j * cw:(j + 1) * cw, :], preferred_element_type=jnp.float32)
        part_u = jnp.dot(block, uv[j * cw:(j + 1) * cw, :], preferred_element_type=jnp.float32)
        if j == 0:
            acc_g[base:base + rows, :] = part_g
            acc_u[base:base + rows, :] = part_u
        else:
            acc_g[base:base + rows, :] += part_g
            acc_u[base:base + rows, :] += part_u

    def peer_step(j):
        for s in range(groups):
            remote(send.at[j, s], peer.at[j, s], xs.at[j, s], xr.at[j, s], mate).wait_recv()
        accumulate(peer, j, rows)

    for j in range(chunks):
        for d in offsets:
            source = (gz + groups - d) % groups
            remote(
                send.at[j, source], own.at[j, source], zs.at[j, d], zr.at[j, source], mate
            ).wait_recv()
            copy = remote(
                own.at[j, source], peer.at[j, source], xs.at[j, source], xr.at[j, source], mate
            )
            copy.start()
            pending.append(copy)
        accumulate(own, j, 0)
        if j:
            peer_step(j - 1)
    peer_step(chunks - 1)
    for s in range(groups):
        remote(wsend, wpeer.at[s], xws.at[s], xwr.at[s], mate).wait_recv()

    def hidden_of(base):
        g = acc_g[base:base + rows, :]
        return (g / (1.0 + jnp.exp(-g)) * acc_u[base:base + rows, :]).astype(jnp.bfloat16)

    sub = lax.broadcasted_iota(jnp.int32, (cap, rows), 0)
    lane = lax.broadcasted_iota(jnp.int32, (cap, rows), 1)
    chosen = lane == sub + gz * cap

    def weights_of(buf):
        cols = []
        for s in range(groups):
            row = jnp.where(side == 0, buf[s, 0, 0:1, :], buf[s, 1, 0:1, :])
            cols.append(jnp.sum(jnp.where(chosen, row, 0.0), axis=1, keepdims=True))
        return jnp.concatenate(cols, axis=0)

    w_peer = weights_of(wpeer)
    hid_peer = hidden_of(rows)
    loads[2].wait()
    for j in range(chunks):
        part = jnp.dot(hid_peer, dv[:, j * cw:(j + 1) * cw], preferred_element_type=jnp.float32)
        pout[j] = (part * w_peer).astype(jnp.bfloat16)
        copy = remote(pout.at[j], pin.at[j], bxs.at[j], bxr.at[j], mate)
        copy.start()
        pending.append(copy)
    w_own = weights_of(wown)
    hid_own = hidden_of(0)
    for j in range(chunks):
        part = jnp.dot(hid_own, dv[:, j * cw:(j + 1) * cw], preferred_element_type=jnp.float32)
        remote(pout.at[j], pin.at[j], bxs.at[j], bxr.at[j], mate).wait_recv()
        total = part * w_own + pin[j].astype(jnp.float32)
        comb[j] = total.astype(jnp.bfloat16).reshape(groups, cap, cw)
        for d in offsets:
            target = (gz + d) % groups
            copy = remote(
                comb.at[j, target], ret.at[j, gz], bzs.at[j, d], bzr.at[j, gz], target * 2 + side
            )
            copy.start()
            pending.append(copy)
        ret[j, pl.ds(gz, 1)] = comb[j, pl.ds(gz, 1)]
    for j in range(chunks):
        for d in offsets:
            source = (gz + groups - d) % groups
            remote(
                comb.at[j, source], ret.at[j, source], bzs.at[j, d], bzr.at[j, source], mate
            ).wait_recv()
        back = jnp.dot(spread_b, ret[j].reshape(rows, cw), preferred_element_type=jnp.float32)
        cols = slice(j * cw, (j + 1) * cw)
        out_ref[:, cols] = (stream_ref[:, cols].astype(jnp.float32) + back).astype(jnp.bfloat16)
    for copy in pending:
        copy.wait_send()


def pair_routed(routes, gate_weight):
    count = lax.axis_size("sp")
    experts = count * gate_weight.shape[0]
    return (
        gate_weight.shape[0] == 1
        and routes.shape[1] == 2
        and experts == 2 * GROUPS
    )


def mixture(stream, norm_gain, routes, route_weights, gate_weight, up_weight, down_weight):
    rows, width = stream.shape
    ff = gate_weight.shape[2]
    groups = lax.axis_size("sp") // 2
    cap, cw = rows // groups, width // CHUNKS
    bf, f32 = jnp.bfloat16, jnp.float32
    quad = pltpu.VMEM((CHUNKS, groups, cap, cw), bf)
    flat = pltpu.VMEM((CHUNKS, rows, cw), bf)
    dma = pltpu.SemaphoreType.DMA
    vm = pl.BlockSpec(memory_space=pltpu.VMEM)
    hbm = pl.BlockSpec(memory_space=pl.ANY)
    return pl.pallas_call(
        functools.partial(moe_kernel, groups, CHUNKS),
        out_shape=jax.ShapeDtypeStruct((rows, width), bf),
        in_specs=[vm] * 4 + [hbm] * 3,
        out_specs=vm,
        scratch_shapes=[
            quad, quad, quad, flat, flat, quad, quad,
            pltpu.VMEM((2, 8, rows), f32),
            pltpu.VMEM((groups, 2, 8, rows), f32),
            pltpu.VMEM((groups, 2, 8, rows), f32),
            pltpu.VMEM((width, ff), bf), pltpu.VMEM((width, ff), bf), pltpu.VMEM((ff, width), bf),
            pltpu.VMEM((2 * rows, ff), f32), pltpu.VMEM((2 * rows, ff), f32),
            dma((CHUNKS, groups)), dma((CHUNKS, groups)), dma((CHUNKS, groups)), dma((CHUNKS, groups)),
            dma((groups,)), dma((groups,)), dma((groups,)), dma((groups,)),
            dma((CHUNKS, groups)), dma((CHUNKS, groups)), dma((CHUNKS,)), dma((CHUNKS,)),
            dma((3,)),
        ],
        compiler_params=pltpu.CompilerParams(
            collective_id=3, has_side_effects=True, vmem_limit_bytes=48 * 1024 * 1024
        ),
        name="mixture",
    )(stream, norm_gain[None, :], routes, route_weights, gate_weight, up_weight, down_weight)


def per_device(
    queries,
    key_rows,
    value_rows,
    doc_ids,
    sink_logit,
    residual,
    out_weight,
    norm_gain,
    gate_weight,
    up_weight,
    down_weight,
    routes,
    route_weights,
):
    local_rows = queries.shape[0]
    anchor = lax.axis_index("sp") * local_rows
    extent = local_rows * lax.axis_size("sp")
    doc_float = doc_ids.astype(jnp.bfloat16)
    block_rows = min(512, local_rows)
    padded_keys, padded_values, padded_docs = fetch_margins(key_rows, value_rows, doc_float)
    block_parts = []
    for row_start in range(0, local_rows, block_rows):
        key_end = row_start + block_rows + 2 * WINDOW
        block_parts.append(
            attend(
                queries[row_start : row_start + block_rows],
                padded_keys[row_start:key_end],
                padded_values[row_start:key_end],
                doc_float[row_start : row_start + block_rows],
                padded_docs[row_start:key_end],
                anchor + row_start,
                anchor + row_start - WINDOW,
                sink_logit,
                extent,
            )
        )
    attended = jnp.concatenate(block_parts, axis=0)
    regrouped = lax.all_to_all(attended, "tp", split_axis=0, concat_axis=1, tiled=True)
    shard_rows = out_weight.shape[0]
    initial = jnp.zeros((regrouped.shape[0], out_weight.shape[1]), jnp.float32)
    running = initial
    weight_piece = lax.all_gather(out_weight, "tp", axis=0, tiled=True)
    for shard_index in range(weight_piece.shape[0] // shard_rows):
        columns = lax.dynamic_slice_in_dim(regrouped, shard_index * shard_rows, shard_rows, 1)
        partial_value = jnp.dot(
            columns,
            weight_piece[shard_index * shard_rows : (shard_index + 1) * shard_rows],
            preferred_element_type=jnp.float32,
        )
        running = running + partial_value.astype(jnp.bfloat16).astype(jnp.float32)
    stream = (residual.astype(jnp.float32) + running).astype(jnp.bfloat16)
    if pair_routed(routes, gate_weight):
        return mixture(
            stream, norm_gain, routes, route_weights, gate_weight, up_weight, down_weight
        )
    stream_f = stream.astype(jnp.float32)
    scale = lax.rsqrt(jnp.mean(stream_f * stream_f, axis=1, keepdims=True) + eps_norm)
    normed = (stream_f * scale * norm_gain[None, :]).astype(jnp.bfloat16)
    home_rows = normed.shape[0]
    width = normed.shape[1]
    route_count = routes.shape[1]
    expert_count = lax.axis_size("sp") * gate_weight.shape[0]
    capacity = route_count * home_rows // expert_count
    flat_routes = routes.reshape(-1)
    one_hot = (flat_routes[:, None] == jnp.arange(expert_count, dtype=jnp.int32)[None, :]).astype(
        jnp.int32
    )
    earlier = jnp.cumsum(one_hot, axis=0) - one_hot
    slot_rank = jnp.sum(earlier * one_hot, axis=1)
    slot_index = flat_routes * capacity + slot_rank
    source_row = (
        jnp.zeros((expert_count * capacity,), jnp.int32)
        .at[slot_index]
        .set(jnp.arange(home_rows * route_count, dtype=jnp.int32) // route_count)
    )
    outgoing = normed[source_row].reshape(expert_count, capacity, width)
    incoming = lax.all_to_all(outgoing, "sp", split_axis=0, concat_axis=0, tiled=True)
    flat_rows = incoming.reshape(-1, width)
    gate_act = jnp.dot(flat_rows, gate_weight[0], preferred_element_type=jnp.float32)
    up_act = jnp.dot(flat_rows, up_weight[0], preferred_element_type=jnp.float32)
    hidden = (jax.nn.silu(gate_act) * up_act).astype(jnp.bfloat16)
    produced = jnp.dot(hidden, down_weight[0], preferred_element_type=jnp.float32).astype(
        jnp.bfloat16
    )
    returned = lax.all_to_all(
        produced.reshape(incoming.shape), "sp", split_axis=0, concat_axis=0, tiled=True
    )
    route_out = returned.reshape(-1, width)[slot_index].reshape(home_rows, route_count, width)
    weighted = jnp.sum(route_weights[:, :, None] * route_out.astype(jnp.float32), axis=1)
    return (stream_f + weighted).astype(jnp.bfloat16)


def solution(mesh):
    return jax.shard_map(
        per_device,
        mesh=mesh,
        in_specs=(
            P("sp", "tp"),
            P("sp", "tp"),
            P("sp", "tp"),
            P("sp"),
            P("tp"),
            P(("sp", "tp"), None),
            P("tp", None),
            P(),
            P("sp", None, None),
            P("sp", None, None),
            P("sp", None, None),
            P(("sp", "tp"), None),
            P(("sp", "tp"), None),
        ),
        out_specs=P(("sp", "tp"), None),
        check_vma=False,
    )
```

```python
import functools

import jax
import jax.numpy as jnp
from jax import lax
from jax.experimental import pallas as pl
from jax.experimental.pallas import tpu as pltpu
from jax.sharding import PartitionSpec as P

HD = 64
WINDOW = 128
GROUPS = 4
CHUNKS = 4


neg_fill = -1e30
eps_norm = 1e-06


def extended(block, sides, width):
    for axis, dim in sides:
        count = lax.axis_size(axis)
        forward = [(i, i + 1) for i in range(count - 1)]
        backward = [(target, source) for source, target in forward]
        low = lax.ppermute(
            lax.slice_in_dim(block, block.shape[dim] - width, None, axis=dim), axis, forward
        )
        high = lax.ppermute(lax.slice_in_dim(block, 0, width, axis=dim), axis, backward)
        block = jnp.concatenate([low, block, high], axis=dim)
    return block


def attend(
    query_part,
    key_part,
    value_part,
    query_docs,
    key_docs,
    query_start,
    key_start,
    sink_logit,
    extent,
):
    query_count = query_part.shape[0]
    key_count = key_part.shape[0]
    groups = key_part.shape[1] // HD
    head_ratio = sink_logit.shape[0] // groups
    query_heads = query_part.reshape(query_count, groups, head_ratio, HD)
    key_heads = key_part.reshape(key_count, groups, HD)
    value_heads = value_part.reshape(key_count, groups, HD)
    scores = jnp.einsum(
        "qgrd,kgd->grqk", query_heads, key_heads, preferred_element_type=jnp.float32
    ) * HD ** (-0.5)
    query_pos = query_start + jnp.arange(query_count, dtype=jnp.int32)
    key_pos = key_start + jnp.arange(key_count, dtype=jnp.int32)
    inside = (key_pos >= 0) & (key_pos < extent)
    allowed = (
        (jnp.abs(query_pos[:, None] - key_pos[None, :]) <= WINDOW)
        & (query_docs[:, None] == key_docs[None, :])
        & inside[None, :]
    )
    masked = jnp.where(allowed[None, None], scores, neg_fill)
    sink_col = sink_logit.reshape(groups, head_ratio)[:, :, None, None]
    row_top = jnp.maximum(jnp.max(masked, axis=3, keepdims=True), sink_col)
    exponent = jnp.where(allowed[None, None], jnp.exp(masked - row_top), 0.0)
    denominator = jnp.sum(exponent, axis=3, keepdims=True) + jnp.exp(sink_col - row_top)
    attn_weight = (exponent / denominator).astype(jnp.bfloat16)
    attended = jnp.einsum(
        "grqk,kgd->qgrd", attn_weight, value_heads, preferred_element_type=jnp.float32
    )
    return attended.astype(jnp.bfloat16).reshape(query_count, -1)


def fetch_margins(key_rows, value_rows, doc_float):
    return (
        extended(key_rows, (("sp", 0),), WINDOW),
        extended(value_rows, (("sp", 0),), WINDOW),
        extended(doc_float, (("sp", 0),), WINDOW),
    )


def moe_kernel(
    groups, chunks,
    stream_ref, gain_ref, routes_ref, rw_ref, gate_hbm, up_hbm, down_hbm,
    out_ref,
    send, own, peer, pout, pin, comb, ret, wsend, wown, wpeer,
    gv, uv, dv, acc_g, acc_u,
    zs, zr, xs, xr, zws, zwr, xws, xwr, bzs, bzr, bxs, bxr, wsem,
):
    me = lax.axis_index("sp")
    gz = me // 2
    side = me % 2
    mate = gz * 2 + 1 - side
    rows, width = stream_ref.shape
    cap = rows // groups
    cw = width // chunks
    half = groups // 2
    offsets = [half] + [d for d in range(groups - 1, 0, -1) if d != half]

    def remote(src, dst, ss, rs, target):
        return pltpu.make_async_remote_copy(
            src_ref=src, dst_ref=dst, send_sem=ss, recv_sem=rs,
            device_id={"sp": target}, device_id_type=pl.DeviceIdType.MESH,
        )

    barrier = pltpu.get_barrier_semaphore()
    for d in offsets:
        pl.semaphore_signal(
            barrier, inc=1, device_id={"sp": ((gz + d) % groups) * 2 + side},
            device_id_type=pl.DeviceIdType.MESH,
        )
    pl.semaphore_signal(
        barrier, inc=1, device_id={"sp": mate}, device_id_type=pl.DeviceIdType.MESH
    )
    loads = [
        pltpu.make_async_copy(s.at[0], t, wsem.at[i])
        for i, (s, t) in enumerate(((gate_hbm, gv), (up_hbm, uv), (down_hbm, dv)))
    ]
    for load in loads:
        load.start()

    stream_f = stream_ref[...].astype(jnp.float32)
    scale = lax.rsqrt(jnp.mean(stream_f * stream_f, axis=1, keepdims=True) + eps_norm)
    normed = (stream_f * scale * gain_ref[...]).astype(jnp.bfloat16)

    first = routes_ref[:, 0:1]
    group_of = first // 2
    lanes = lax.broadcasted_iota(jnp.int32, (rows, 128), 1)
    one_hot = jnp.where(group_of == lanes, 1.0, 0.0)
    ri = lax.broadcasted_iota(jnp.int32, (rows, rows), 0)
    ci = lax.broadcasted_iota(jnp.int32, (rows, rows), 1)
    below = jnp.where(ci < ri, 1.0, 0.0).astype(jnp.bfloat16)
    ranks = jnp.dot(below, one_hot.astype(jnp.bfloat16), preferred_element_type=jnp.float32)
    slot = group_of.astype(jnp.float32) * cap + jnp.sum(ranks * one_hot, axis=1, keepdims=True)
    spread = jnp.where(slot == ci.astype(jnp.float32), 1.0, 0.0)
    spread_b = spread.astype(jnp.bfloat16)
    slot_lane = jnp.sum(jnp.where(ri == ci, slot, 0.0), axis=0, keepdims=True)
    pick = jnp.where(ri.astype(jnp.float32) == slot_lane, 1.0, 0.0).astype(jnp.bfloat16)
    for parity in range(2):
        w_col = jnp.where(first % 2 == parity, rw_ref[:, 0:1], rw_ref[:, 1:2])
        w_row = jnp.sum(spread * w_col, axis=0, keepdims=True)
        wsend[parity] = jnp.broadcast_to(w_row, (8, rows))

    pl.semaphore_wait(barrier, groups)

    pending = []
    for d in offsets:
        copy = remote(wsend, wown.at[gz], zws.at[d], zwr.at[gz], ((gz + d) % groups) * 2 + side)
        copy.start()
        pending.append(copy)
    copy = remote(wsend, wpeer.at[gz], xws.at[gz], xwr.at[gz], mate)
    copy.start()
    pending.append(copy)

    for j in range(chunks):
        piece = jnp.dot(pick, normed[:, j * cw:(j + 1) * cw], preferred_element_type=jnp.float32)
        send[j] = piece.astype(jnp.bfloat16).reshape(groups, cap, cw)
        for d in offsets:
            target = (gz + d) % groups
            copy = remote(
                send.at[j, target], own.at[j, gz], zs.at[j, d], zr.at[j, gz], target * 2 + side
            )
            copy.start()
            pending.append(copy)
        copy = remote(send.at[j, gz], peer.at[j, gz], xs.at[j, gz], xr.at[j, gz], mate)
        copy.start()
        pending.append(copy)
        own[j, pl.ds(gz, 1)] = send[j, pl.ds(gz, 1)]
    wown[pl.ds(gz, 1)] = wsend[...][None]

    for d in offsets:
        source = (gz + groups - d) % groups
        remote(wsend, wown.at[source], zws.at[d], zwr.at[source], mate).wait_recv()
        copy = remote(wown.at[source], wpeer.at[source], xws.at[source], xwr.at[source], mate)
        copy.start()
        pending.append(copy)

    loads[0].wait()
    loads[1].wait()

    def accumulate(buf, j, base):
        block = buf[j].reshape(rows, cw)
        part_g = jnp.dot(block, gv[j * cw:(j + 1) * cw, :], preferred_element_type=jnp.float32)
        part_u = jnp.dot(block, uv[j * cw:(j + 1) * cw, :], preferred_element_type=jnp.float32)
        if j == 0:
            acc_g[base:base + rows, :] = part_g
            acc_u[base:base + rows, :] = part_u
        else:
            acc_g[base:base + rows, :] += part_g
            acc_u[base:base + rows, :] += part_u

    def peer_step(j):
        for s in range(groups):
            remote(send.at[j, s], peer.at[j, s], xs.at[j, s], xr.at[j, s], mate).wait_recv()
        accumulate(peer, j, rows)

    for j in range(chunks):
        for d in offsets:
            source = (gz + groups - d) % groups
            remote(
                send.at[j, source], own.at[j, source], zs.at[j, d], zr.at[j, source], mate
            ).wait_recv()
            copy = remote(
                own.at[j, source], peer.at[j, source], xs.at[j, source], xr.at[j, source], mate
            )
            copy.start()
            pending.append(copy)
        accumulate(own, j, 0)
        if j:
            peer_step(j - 1)
    peer_step(chunks - 1)
    for s in range(groups):
        remote(wsend, wpeer.at[s], xws.at[s], xwr.at[s], mate).wait_recv()

    def hidden_of(base):
        g = acc_g[base:base + rows, :]
        return (g / (1.0 + jnp.exp(-g)) * acc_u[base:base + rows, :]).astype(jnp.bfloat16)

    sub = lax.broadcasted_iota(jnp.int32, (cap, rows), 0)
    lane = lax.broadcasted_iota(jnp.int32, (cap, rows), 1)
    chosen = lane == sub + gz * cap

    def weights_of(buf):
        cols = []
        for s in range(groups):
            row = jnp.where(side == 0, buf[s, 0, 0:1, :], buf[s, 1, 0:1, :])
            cols.append(jnp.sum(jnp.where(chosen, row, 0.0), axis=1, keepdims=True))
        return jnp.concatenate(cols, axis=0)

    w_peer = weights_of(wpeer)
    hid_peer = hidden_of(rows)
    loads[2].wait()
    for j in range(chunks):
        part = jnp.dot(hid_peer, dv[:, j * cw:(j + 1) * cw], preferred_element_type=jnp.float32)
        pout[j] = (part * w_peer).astype(jnp.bfloat16)
        copy = remote(pout.at[j], pin.at[j], bxs.at[j], bxr.at[j], mate)
        copy.start()
        pending.append(copy)
    w_own = weights_of(wown)
    hid_own = hidden_of(0)
    for j in range(chunks):
        part = jnp.dot(hid_own, dv[:, j * cw:(j + 1) * cw], preferred_element_type=jnp.float32)
        remote(pout.at[j], pin.at[j], bxs.at[j], bxr.at[j], mate).wait_recv()
        total = part * w_own + pin[j].astype(jnp.float32)
        comb[j] = total.astype(jnp.bfloat16).reshape(groups, cap, cw)
        for d in offsets:
            target = (gz + d) % groups
            copy = remote(
                comb.at[j, target], ret.at[j, gz], bzs.at[j, d], bzr.at[j, gz], target * 2 + side
            )
            copy.start()
            pending.append(copy)
        ret[j, pl.ds(gz, 1)] = comb[j, pl.ds(gz, 1)]
    for j in range(chunks):
        for d in offsets:
            source = (gz + groups - d) % groups
            remote(
                comb.at[j, source], ret.at[j, source], bzs.at[j, d], bzr.at[j, source], mate
            ).wait_recv()
        back = jnp.dot(spread_b, ret[j].reshape(rows, cw), preferred_element_type=jnp.float32)
        cols = slice(j * cw, (j + 1) * cw)
        out_ref[:, cols] = (stream_ref[:, cols].astype(jnp.float32) + back).astype(jnp.bfloat16)
    for copy in pending:
        copy.wait_send()


def front_kernel(
    chunks,
    sink_ref, q_ref, k_ref, v_ref, doc_ref, res_ref, w_ref,
    out_ref,
    kx, vx, dl, dr, dx, att, am_far, am_near, w_mate, acc, ysend, yrecv,
    hs, hr, ms, mr, ys, yr,
):
    sp = lax.axis_index("sp")
    tp = lax.axis_index("tp")
    sp_count = lax.axis_size("sp")
    mate = tp + 1 - 2 * (tp % 2)
    across = (tp + 2) % 4
    mate_across = (mate + 2) % 4
    after = (sp + 1) % sp_count
    before = (sp + sp_count - 1) % sp_count
    blocks = q_ref.shape[0] // WINDOW
    home_blocks = blocks // 4
    half = blocks // 2
    kv_heads = k_ref.shape[1] // HD
    ratio = q_ref.shape[1] // k_ref.shape[1]
    width = out_ref.shape[1]
    cw = width // chunks
    f32, bf = jnp.float32, jnp.bfloat16
    mesh_id = pl.DeviceIdType.MESH

    def remote(src, dst, ss, rs, where):
        return pltpu.make_async_remote_copy(
            src_ref=src, dst_ref=dst, send_sem=ss, recv_sem=rs,
            device_id=where, device_id_type=mesh_id,
        )

    barrier = pltpu.get_barrier_semaphore()
    for where in ({"sp": after}, {"sp": before}, {"tp": mate}, {"tp": across}):
        pl.semaphore_signal(barrier, inc=1, device_id=where, device_id_type=mesh_id)
    for b in range(blocks):
        kx[b + 1] = k_ref[b * WINDOW:(b + 1) * WINDOW, :]
        vx[b + 1] = v_ref[b * WINDOW:(b + 1) * WINDOW, :]
        dx[b + 1] = jnp.broadcast_to(doc_ref[b:b + 1, :].astype(f32), (8, WINDOW))
    pl.semaphore_wait(barrier, 4)

    tail = pl.ds((blocks - 1) * WINDOW, WINDOW)
    lead = pl.ds(0, WINDOW)
    halo = [
        remote(k_ref.at[tail], kx.at[0], hs.at[0], hr.at[0], {"sp": after}),
        remote(v_ref.at[tail], vx.at[0], hs.at[1], hr.at[1], {"sp": after}),
        remote(doc_ref, dl, hs.at[2], hr.at[2], {"sp": after}),
        remote(k_ref.at[lead], kx.at[blocks + 1], hs.at[3], hr.at[3], {"sp": before}),
        remote(v_ref.at[lead], vx.at[blocks + 1], hs.at[4], hr.at[4], {"sp": before}),
        remote(doc_ref, dr, hs.at[5], hr.at[5], {"sp": before}),
    ]
    for copy in halo:
        copy.start()
    w_copy = remote(w_ref, w_mate, ms.at[0], mr.at[0], {"tp": mate})
    w_copy.start()

    qi = lax.broadcasted_iota(jnp.int32, (WINDOW, 3 * WINDOW), 0)
    ki = lax.broadcasted_iota(jnp.int32, (WINDOW, 3 * WINDOW), 1)
    band = (ki >= qi) & (ki <= qi + 2 * WINDOW)
    eye = lax.broadcasted_iota(jnp.int32, (WINDOW, WINDOW), 0) == lax.broadcasted_iota(
        jnp.int32, (WINDOW, WINDOW), 1
    )

    def attend_block(b):
        own_docs = dx[b + 1][0:1]
        key_docs = jnp.concatenate([dx[b][0:1], own_docs, dx[b + 2][0:1]], axis=1)
        query_docs = jnp.sum(jnp.where(eye, own_docs, 0.0), axis=1, keepdims=True)
        bias = jnp.where(band & (key_docs == query_docs), 0.0, neg_fill)
        keys = kx[pl.ds(b, 3)].reshape(3 * WINDOW, kv_heads * HD)
        values = vx[pl.ds(b, 3)].reshape(3 * WINDOW, kv_heads * HD)
        home = b // home_blocks
        to_rows = pl.ds(pl.multiple_of((b % home_blocks) * WINDOW, WINDOW), WINDOW)
        from_rows = pl.ds(pl.multiple_of(b * WINDOW, WINDOW), WINDOW)
        for g in range(kv_heads):
            span = slice(g * ratio * HD, (g + 1) * ratio * HD)
            q = q_ref[from_rows, span] * jnp.asarray(HD ** (-0.5), bf)
            stacked = jnp.concatenate([q[:, r * HD:(r + 1) * HD] for r in range(ratio)], axis=0)
            scores = lax.dot_general(
                stacked, keys[:, g * HD:(g + 1) * HD], (((1,), (1,)), ((), ())),
                preferred_element_type=f32,
            )
            vg = values[:, g * HD:(g + 1) * HD]
            parts = []
            for r in range(ratio):
                sink = sink_ref[g * ratio + r]
                s = scores[r * WINDOW:(r + 1) * WINDOW] + bias
                top = jnp.maximum(jnp.max(s, axis=1, keepdims=True), sink)
                e = jnp.exp(s - top)
                den = jnp.sum(e, axis=1, keepdims=True) + jnp.exp(sink - top)
                o = jnp.dot(e.astype(bf), vg, preferred_element_type=f32)
                parts.append((o / den).astype(bf))
            att[home, to_rows, span] = jnp.concatenate(parts, axis=1)

    def far_step(i, carry):
        @pl.when(i == half - 1)
        def _():
            for copy in halo:
                copy.wait_recv()
            left = dl[blocks - 1:blocks, :].astype(f32)
            right = dr[0:1, :].astype(f32)
            left = jnp.where(sp == 0, -1.0, left)
            right = jnp.where(sp == sp_count - 1, -1.0, right)
            dx[0] = jnp.broadcast_to(left, (8, WINDOW))
            dx[blocks + 1] = jnp.broadcast_to(right, (8, WINDOW))

        attend_block(jnp.where(tp < 2, half + i, half - 1 - i))
        return carry

    lax.fori_loop(0, half, far_step, 0)
    far_copy = remote(att.at[mate_across], am_far, ms.at[1], mr.at[1], {"tp": mate})
    far_copy.start()
    w_copy.wait_recv()
    far_copy.wait_recv()
    sent = []
    for c in range(chunks):
        cols = slice(c * cw, (c + 1) * cw)
        part = jnp.dot(att[across], w_ref[:, cols], preferred_element_type=f32)
        part += jnp.dot(am_far[...], w_mate[:, cols], preferred_element_type=f32)
        ysend[c] = part.astype(bf)
        copy = remote(ysend.at[c], yrecv.at[c], ys.at[c], yr.at[c], {"tp": across})
        copy.start()
        sent.append(copy)

    def near_step(i, carry):
        attend_block(jnp.where(tp < 2, half - 1 - i, half + i))
        return carry

    lax.fori_loop(0, half, near_step, 0)
    near_copy = remote(att.at[mate], am_near, ms.at[2], mr.at[2], {"tp": mate})
    near_copy.start()
    near_copy.wait_recv()
    for c in range(chunks):
        cols = slice(c * cw, (c + 1) * cw)
        part = jnp.dot(att[tp], w_ref[:, cols], preferred_element_type=f32)
        part += jnp.dot(am_near[...], w_mate[:, cols], preferred_element_type=f32)
        acc[:, cols] = part + res_ref[:, cols].astype(f32)
    for c in range(chunks):
        cols = slice(c * cw, (c + 1) * cw)
        sent[c].wait_recv()
        out_ref[:, cols] = (acc[:, cols] + yrecv[c].astype(f32)).astype(bf)
    for copy in halo + [w_copy, far_copy, near_copy] + sent:
        copy.wait_send()


def front(queries, key_rows, value_rows, doc_ids, sink_logit, residual, out_weight):
    rows, width = residual.shape
    local, heads_width = queries.shape
    kv_width = key_rows.shape[1]
    blocks = local // WINDOW
    bf, f32 = jnp.bfloat16, jnp.float32
    dma = pltpu.SemaphoreType.DMA
    vm = pl.BlockSpec(memory_space=pltpu.VMEM)
    docs = doc_ids.reshape(blocks, WINDOW)
    return pl.pallas_call(
        functools.partial(front_kernel, CHUNKS),
        out_shape=jax.ShapeDtypeStruct((rows, width), bf),
        in_specs=[pl.BlockSpec(memory_space=pltpu.SMEM)] + [vm] * 6,
        out_specs=vm,
        scratch_shapes=[
            pltpu.VMEM((blocks + 2, WINDOW, kv_width), bf),
            pltpu.VMEM((blocks + 2, WINDOW, kv_width), bf),
            pltpu.VMEM((blocks, WINDOW), jnp.int32),
            pltpu.VMEM((blocks, WINDOW), jnp.int32),
            pltpu.VMEM((blocks + 2, 8, WINDOW), f32),
            pltpu.VMEM((4, rows, heads_width), bf),
            pltpu.VMEM((rows, heads_width), bf),
            pltpu.VMEM((rows, heads_width), bf),
            pltpu.VMEM(out_weight.shape, bf),
            pltpu.VMEM((rows, width), f32),
            pltpu.VMEM((CHUNKS, rows, width // CHUNKS), bf),
            pltpu.VMEM((CHUNKS, rows, width // CHUNKS), bf),
            dma((6,)), dma((6,)), dma((3,)), dma((3,)), dma((CHUNKS,)), dma((CHUNKS,)),
        ],
        compiler_params=pltpu.CompilerParams(
            collective_id=4, has_side_effects=True, vmem_limit_bytes=48 * 1024 * 1024
        ),
        name="front",
    )(sink_logit, queries, key_rows, value_rows, docs, residual, out_weight)


def pair_routed(routes, gate_weight):
    count = lax.axis_size("sp")
    experts = count * gate_weight.shape[0]
    return (
        gate_weight.shape[0] == 1
        and routes.shape[1] == 2
        and experts == 2 * GROUPS
    )


def mixture(stream, norm_gain, routes, route_weights, gate_weight, up_weight, down_weight):
    rows, width = stream.shape
    ff = gate_weight.shape[2]
    groups = lax.axis_size("sp") // 2
    cap, cw = rows // groups, width // CHUNKS
    bf, f32 = jnp.bfloat16, jnp.float32
    quad = pltpu.VMEM((CHUNKS, groups, cap, cw), bf)
    flat = pltpu.VMEM((CHUNKS, rows, cw), bf)
    dma = pltpu.SemaphoreType.DMA
    vm = pl.BlockSpec(memory_space=pltpu.VMEM)
    hbm = pl.BlockSpec(memory_space=pl.ANY)
    return pl.pallas_call(
        functools.partial(moe_kernel, groups, CHUNKS),
        out_shape=jax.ShapeDtypeStruct((rows, width), bf),
        in_specs=[vm] * 4 + [hbm] * 3,
        out_specs=vm,
        scratch_shapes=[
            quad, quad, quad, flat, flat, quad, quad,
            pltpu.VMEM((2, 8, rows), f32),
            pltpu.VMEM((groups, 2, 8, rows), f32),
            pltpu.VMEM((groups, 2, 8, rows), f32),
            pltpu.VMEM((width, ff), bf), pltpu.VMEM((width, ff), bf), pltpu.VMEM((ff, width), bf),
            pltpu.VMEM((2 * rows, ff), f32), pltpu.VMEM((2 * rows, ff), f32),
            dma((CHUNKS, groups)), dma((CHUNKS, groups)), dma((CHUNKS, groups)), dma((CHUNKS, groups)),
            dma((groups,)), dma((groups,)), dma((groups,)), dma((groups,)),
            dma((CHUNKS, groups)), dma((CHUNKS, groups)), dma((CHUNKS,)), dma((CHUNKS,)),
            dma((3,)),
        ],
        compiler_params=pltpu.CompilerParams(
            collective_id=3, has_side_effects=True, vmem_limit_bytes=48 * 1024 * 1024
        ),
        name="mixture",
    )(stream, norm_gain[None, :], routes, route_weights, gate_weight, up_weight, down_weight)


def stream_of(
    queries, key_rows, value_rows, doc_ids, sink_logit, residual, out_weight
):
    local_rows = queries.shape[0]
    if lax.axis_size("tp") == 4 and local_rows % (8 * WINDOW) == 0:
        return front(queries, key_rows, value_rows, doc_ids, sink_logit, residual, out_weight)
    anchor = lax.axis_index("sp") * local_rows
    extent = local_rows * lax.axis_size("sp")
    doc_float = doc_ids.astype(jnp.bfloat16)
    block_rows = min(512, local_rows)
    padded_keys, padded_values, padded_docs = fetch_margins(key_rows, value_rows, doc_float)
    block_parts = []
    for row_start in range(0, local_rows, block_rows):
        key_end = row_start + block_rows + 2 * WINDOW
        block_parts.append(
            attend(
                queries[row_start : row_start + block_rows],
                padded_keys[row_start:key_end],
                padded_values[row_start:key_end],
                doc_float[row_start : row_start + block_rows],
                padded_docs[row_start:key_end],
                anchor + row_start,
                anchor + row_start - WINDOW,
                sink_logit,
                extent,
            )
        )
    attended = jnp.concatenate(block_parts, axis=0)
    regrouped = lax.all_to_all(attended, "tp", split_axis=0, concat_axis=1, tiled=True)
    shard_rows = out_weight.shape[0]
    initial = jnp.zeros((regrouped.shape[0], out_weight.shape[1]), jnp.float32)
    running = initial
    weight_piece = lax.all_gather(out_weight, "tp", axis=0, tiled=True)
    for shard_index in range(weight_piece.shape[0] // shard_rows):
        columns = lax.dynamic_slice_in_dim(regrouped, shard_index * shard_rows, shard_rows, 1)
        partial_value = jnp.dot(
            columns,
            weight_piece[shard_index * shard_rows : (shard_index + 1) * shard_rows],
            preferred_element_type=jnp.float32,
        )
        running = running + partial_value.astype(jnp.bfloat16).astype(jnp.float32)
    stream = (residual.astype(jnp.float32) + running).astype(jnp.bfloat16)
    return stream


def per_device(
    queries,
    key_rows,
    value_rows,
    doc_ids,
    sink_logit,
    residual,
    out_weight,
    norm_gain,
    gate_weight,
    up_weight,
    down_weight,
    routes,
    route_weights,
):
    stream = stream_of(
        queries, key_rows, value_rows, doc_ids, sink_logit, residual, out_weight
    )
    if pair_routed(routes, gate_weight):
        return mixture(
            stream, norm_gain, routes, route_weights, gate_weight, up_weight, down_weight
        )
    stream_f = stream.astype(jnp.float32)
    scale = lax.rsqrt(jnp.mean(stream_f * stream_f, axis=1, keepdims=True) + eps_norm)
    normed = (stream_f * scale * norm_gain[None, :]).astype(jnp.bfloat16)
    home_rows = normed.shape[0]
    width = normed.shape[1]
    route_count = routes.shape[1]
    expert_count = lax.axis_size("sp") * gate_weight.shape[0]
    capacity = route_count * home_rows // expert_count
    flat_routes = routes.reshape(-1)
    one_hot = (flat_routes[:, None] == jnp.arange(expert_count, dtype=jnp.int32)[None, :]).astype(
        jnp.int32
    )
    earlier = jnp.cumsum(one_hot, axis=0) - one_hot
    slot_rank = jnp.sum(earlier * one_hot, axis=1)
    slot_index = flat_routes * capacity + slot_rank
    source_row = (
        jnp.zeros((expert_count * capacity,), jnp.int32)
        .at[slot_index]
        .set(jnp.arange(home_rows * route_count, dtype=jnp.int32) // route_count)
    )
    outgoing = normed[source_row].reshape(expert_count, capacity, width)
    incoming = lax.all_to_all(outgoing, "sp", split_axis=0, concat_axis=0, tiled=True)
    flat_rows = incoming.reshape(-1, width)
    gate_act = jnp.dot(flat_rows, gate_weight[0], preferred_element_type=jnp.float32)
    up_act = jnp.dot(flat_rows, up_weight[0], preferred_element_type=jnp.float32)
    hidden = (jax.nn.silu(gate_act) * up_act).astype(jnp.bfloat16)
    produced = jnp.dot(hidden, down_weight[0], preferred_element_type=jnp.float32).astype(
        jnp.bfloat16
    )
    returned = lax.all_to_all(
        produced.reshape(incoming.shape), "sp", split_axis=0, concat_axis=0, tiled=True
    )
    route_out = returned.reshape(-1, width)[slot_index].reshape(home_rows, route_count, width)
    weighted = jnp.sum(route_weights[:, :, None] * route_out.astype(jnp.float32), axis=1)
    return (stream_f + weighted).astype(jnp.bfloat16)


def solution(mesh):
    return jax.shard_map(
        per_device,
        mesh=mesh,
        in_specs=(
            P("sp", "tp"),
            P("sp", "tp"),
            P("sp", "tp"),
            P("sp"),
            P("tp"),
            P(("sp", "tp"), None),
            P("tp", None),
            P(),
            P("sp", None, None),
            P("sp", None, None),
            P("sp", None, None),
            P(("sp", "tp"), None),
            P(("sp", "tp"), None),
        ),
        out_specs=P(("sp", "tp"), None),
        check_vma=False,
    )
```
